32 devices in a mesh: sp: 8 (over z, x), tp: 4 (over y, core).
Axes of the slice: x: 2, y: 2, z: 4, core: 2. Of those that a mesh axis runs over, the one named last changes fastest.
Arguments:
- residual: bfloat16 [1536, 2048], P(('sp', 'tp')), may hold values from -6 to 6
- query_a: bfloat16 [1536, 1536], P('sp', 'tp'), may hold values from -600 to 600
- query_b: bfloat16 [1536, 2560], P('sp', 'tp'), may hold values from -600 to 600
- latents: bfloat16 [1536, 512], P('sp'), may hold values from -6 to 6
- rope_key: bfloat16 [1536, 32], P('sp'), may hold values from -6 to 6
- key_up_a: bfloat16 [512, 1024], P(None, 'tp'), may hold values from -0.25 to 0.25
- value_up_a: bfloat16 [512, 1024], P(None, 'tp'), may hold values from -0.25 to 0.25
- key_up_b: bfloat16 [512, 2048], P(None, 'tp'), may hold values from -0.25 to 0.25
- value_up_b: bfloat16 [512, 2048], P(None, 'tp'), may hold values from -0.25 to 0.25
- out_proj_a: bfloat16 [1024, 2048], P('tp'), may hold values from -1.5 to 1.5
- out_proj_b: bfloat16 [2048, 2048], P('tp'), may hold values from -1.5 to 1.5
- norm_gain: float32 [2048], replicated, may hold values from 0.1 to 1.9
- routes: int32 [1536, 2], P('sp'), may hold values from 0 to 7, all different within a row; in each aligned block of 192 rows (0 to 191, 192 to 383, ...) at most 72 rows name the same one
- route_weights: float32 [1536, 2], P('sp'), may hold values from 0.2 to 1
- shared_gate: bfloat16 [2048, 2048], P(None, 'tp'), may hold values from -0.125 to 0.125
- shared_up: bfloat16 [2048, 2048], P(None, 'tp'), may hold values from -0.125 to 0.125
- shared_down: bfloat16 [2048, 2048], P('tp'), may hold values from -0.125 to 0.125
- expert_gate: bfloat16 [8, 2048, 2048], P('sp', None, 'tp'), may hold values from -0.125 to 0.125
- expert_up: bfloat16 [8, 2048, 2048], P('sp', None, 'tp'), may hold values from -0.125 to 0.125
- expert_down: bfloat16 [8, 2048, 2048], P('sp', 'tp'), may hold values from -0.125 to 0.125
Outputs:
- layer_out: bfloat16 [1536, 2048], P(('sp', 'tp'))
The draws below stay inside these ranges and needn't reach their ends.
Inputs may be any that keep to these rules, and one draw needn't show every extreme that they name: `routes`: in each aligned block of 192 rows, no expert is named by more than 72 rows, a bound that some block reaches; a row names 2 different experts.
All inputs are finite; a program needn't handle non-finite values.
Results may differ from the reference program's by a relative error of at most 0.022.
The reference program's roundings to bfloat16 on the way count: a program that leaves them out, or rounds other values in their place, can miss the bound.
Values may be sent and summed in bfloat16 or wider, within the bound.
No kernel may reach another device: no remote copies, remote signals or barrier semaphores. Data moves between devices by JAX's collectives and lax.ppermute only.
A program may use at most 64 MiB of HBM per device.

```python
import math
import jax
import jax.numpy as jnp
import numpy as np
from jax import lax

D = 2048
HA = 16
HB = 16
DA = 64
VA = 64
DB = 128
VB = 128
ROPE = 32
KV_RANK = 512
EXPERT_FF = 2048
SHARED_FF = 2048
TOPK = 2
TOK_DEV = 192
TOKENS = 1536
EXPERTS = 8
CAP = 72
N_SP = 8
N_TP = 4


def drawn_queries(key, width):
    base = jax.random.normal(key, (TOKENS, width), jnp.float32)
    return jnp.clip(base, -600.0, 600.0).astype(jnp.bfloat16)


def draw_query_a(key, part):
    return drawn_queries(jax.random.fold_in(key, 11), HA * (DA + ROPE))


def draw_query_b(key, part):
    return drawn_queries(jax.random.fold_in(key, 23), HB * (DB + ROPE))


def shard_levels(key, shape, cuts, smallest, top_value):
    def one(position, blocks):
        steps = jax.random.uniform(jax.random.fold_in(jax.random.fold_in(key, 6), position), (blocks,), jnp.float32, smallest / len(cuts), top_value / len(cuts))
        return jnp.repeat(jnp.exp(steps), shape[position] // blocks).reshape((-1,) + (1,) * (len(shape) - position - 1))

    loudness = one(*cuts[0])
    for cut in cuts[1:]:
        loudness = loudness * one(*cut)
    return loudness


def shared_out(stream_key, own, number, rows, amount, top, most, slope):
    ranking = jax.random.permutation(stream_key, amount)
    heavy_load, ordinary = load_shares(amount, rows * top, most, slope, True), load_shares(amount, rows * top, most, slope, False)
    places = jnp.arange(amount)

    def named(sizes, offset_by):
        used = int((sizes > 0).sum())
        fixed = max(1, used // 4)
        passed = fixed + (places - fixed + offset_by * (used - fixed)) % max(1, amount - fixed)
        return jnp.zeros((amount,), jnp.int32).at[ranking[jnp.where(places < fixed, places, passed)]].set(jnp.asarray(sizes, jnp.int32))

    sizes = jnp.where(number % 4 == 0, named(heavy_load, number // 4), named(ordinary, number - number // 4 - 1))
    mixed = jax.random.permutation(jax.random.fold_in(own, 3), amount)
    giver, sink = mixed[0:amount // 2 * 2:2], mixed[1:amount // 2 * 2:2]
    slack = jnp.minimum(sizes[giver] - 1, most - sizes[sink]) // 2
    slack = jnp.where((giver == ranking[0]) | (sink == ranking[0]) | (sizes[sink] == 0), 0, jnp.maximum(slack, 0))
    passed = jax.random.randint(jax.random.fold_in(own, 4), (amount // 2,), 0, 1 << 20) % (slack + 1)
    sizes = sizes.at[giver].add(-passed).at[sink].add(passed)
    labels = jnp.searchsorted(jnp.cumsum(sizes), jnp.arange(rows * top), side="right").astype(jnp.int32)
    listing = labels.reshape(top, rows).T
    listing = listing[jax.random.permutation(jax.random.fold_in(own, 1), rows)]
    offset_by = jax.random.randint(jax.random.fold_in(own, 2), (rows, 1), 0, top)
    return jnp.take_along_axis(listing, (jnp.arange(top)[None, :] + offset_by) % top, axis=1)


def load_shares(number_of, total, limit, skew, full):
    loads = [(1 << 20) // math.isqrt(standing ** skew) + 1 for standing in range(1, number_of + 1)]
    largest = limit if full else min(limit, max(-(-total // number_of), total * loads[0] // sum(loads)))
    least = 1 if total - largest >= number_of - 1 else 0
    given, surplus = [largest] + [least] * (number_of - 1), total - largest - least * (number_of - 1)
    while surplus > 0:
        candidates = [i for i in range(1, number_of) if given[i] < largest] or [i for i in range(1, number_of) if given[i] < limit]
        whole, remaining = sum([loads[i] for i in candidates]), surplus
        for i in candidates:
            addition = min(limit - given[i], max(1, remaining * loads[i] // whole), surplus)
            given[i] = given[i] + addition
            surplus = surplus - addition
    return np.array(given)


def bell_draw(stream_key, extent, spread, most, shards=(), kind=jnp.bfloat16):
    gain = shard_levels(stream_key, extent, shards, -0.22, 0.18) if shards else 1.0
    values = jax.random.normal(stream_key, extent, jnp.float32) * spread * gain
    return jnp.minimum(jnp.maximum(values, -most), most).astype(kind)


def setup_inputs(seed: int = 0) -> dict:
    arg_keys = jax.random.split(jax.random.key(seed), 21)
    residual = bell_draw(arg_keys[0], (TOKENS, D), 1.0, 6.0, ((0, 32),))
    query_a = draw_query_a(jax.random.fold_in(arg_keys[20], 71), 0)
    query_b = draw_query_b(jax.random.fold_in(arg_keys[20], 71), 0)
    latents = bell_draw(arg_keys[3], (TOKENS, KV_RANK), 1.0, 6.0, ((0, 8),))
    rope_key = bell_draw(arg_keys[4], (TOKENS, ROPE), 1.0, 6.0, ((0, 8),))
    key_up_a = bell_draw(arg_keys[5], (KV_RANK, HA * DA), KV_RANK ** -0.5, 0.25, ((1, 4),))
    value_up_a = bell_draw(arg_keys[6], (KV_RANK, HA * VA), KV_RANK ** -0.5, 0.25, ((1, 4),))
    key_up_b = bell_draw(arg_keys[7], (KV_RANK, HB * DB), KV_RANK ** -0.5, 0.25, ((1, 4),))
    value_up_b = bell_draw(arg_keys[8], (KV_RANK, HB * VB), KV_RANK ** -0.5, 0.25, ((1, 4),))
    out_proj_a = bell_draw(arg_keys[9], (HA * VA, D), HA ** -0.5, 1.5, ((0, 4),))
    out_proj_b = bell_draw(arg_keys[10], (HB * VB, D), HA ** -0.5, 1.5, ((0, 4),))
    norm_gain = jnp.clip(1.0 + 0.18 * jax.random.normal(arg_keys[11], (D,), jnp.float32), 0.1, 1.9)
    routes_keys = jax.random.split(jax.random.fold_in(arg_keys[12], 1), TOKENS // TOK_DEV)
    routes_turns = jax.random.permutation(jax.random.fold_in(arg_keys[12], 3), TOKENS // TOK_DEV)
    routes = jax.vmap(lambda own, number: shared_out(jax.random.fold_in(arg_keys[12], 2), own, number, TOK_DEV, EXPERTS, TOPK, CAP, 1))(routes_keys, routes_turns).reshape((TOKENS, TOPK))
    route_weights = jnp.clip(0.2 + 0.8 * jax.random.uniform(arg_keys[13], (TOKENS, TOPK), jnp.float32) ** shard_levels(arg_keys[13], (TOKENS, TOPK), ((0, 8),), -0.2, 0.2), 0.2, 1.0)
    shared_gate = bell_draw(arg_keys[14], (D, SHARED_FF), D ** -0.5, 0.125, ((1, 4),))
    shared_up = bell_draw(arg_keys[15], (D, SHARED_FF), D ** -0.5, 0.125, ((1, 4),))
    shared_down = bell_draw(arg_keys[16], (SHARED_FF, D), SHARED_FF ** -0.5, 0.125, ((0, 4),))
    expert_gate = bell_draw(arg_keys[17], (EXPERTS, D, EXPERT_FF), D ** -0.5, 0.125, ((0, 8), (2, 4)))
    expert_up = bell_draw(arg_keys[18], (EXPERTS, D, EXPERT_FF), D ** -0.5, 0.125, ((0, 8), (2, 4)))
    expert_down = bell_draw(arg_keys[19], (EXPERTS, EXPERT_FF, D), EXPERT_FF ** -0.5, 0.125, ((0, 8), (1, 4)))
    return dict(residual=residual, query_a=query_a, query_b=query_b, latents=latents, rope_key=rope_key, key_up_a=key_up_a, value_up_a=value_up_a, key_up_b=key_up_b, value_up_b=value_up_b, out_proj_a=out_proj_a, out_proj_b=out_proj_b, norm_gain=norm_gain, routes=routes, route_weights=route_weights, shared_gate=shared_gate, shared_up=shared_up, shared_down=shared_down, expert_gate=expert_gate, expert_up=expert_up, expert_down=expert_down)


theta_base = 10000.0
norm_eps = 1e-06

def round_trip(values):
    return lax.optimization_barrier(values.astype(jnp.bfloat16)).astype(jnp.float32)

def tables(positions):
    half = ROPE // 2
    freqs = theta_base ** (-(2.0 * jnp.arange(half, dtype=jnp.float32)) / ROPE)
    angles = positions.astype(jnp.float32)[:, None] * freqs[None, :]
    return (jnp.cos(angles), jnp.sin(angles))

def rotate(values, cosine, sine):
    half = values.shape[-1] // 2
    first = values[..., :half].astype(jnp.float32)
    second = values[..., half:].astype(jnp.float32)
    turned = jnp.concatenate([first * cosine - second * sine, first * sine + second * cosine], axis=-1)
    return turned.astype(jnp.bfloat16)

def attend(queries, keys, values, rot_key, heads, nope, vsize, cosine, sine):
    length = queries.shape[0]
    block = math.gcd(length, 512)
    shaped = queries.reshape(length, heads, nope + ROPE)
    q_nope = shaped[..., :nope]
    q_rope = rotate(shaped[..., nope:], cosine[:, None, :], sine[:, None, :])
    key_all = keys.reshape(length, heads, nope).astype(jnp.float32)
    value_all = values.reshape(length, heads, vsize).astype(jnp.float32)
    rot_all = rot_key.astype(jnp.float32)
    scale = (nope + ROPE) ** (-0.5)
    key_pos = jnp.arange(length, dtype=jnp.int32)

    def one_block(index):
        start = (index * block).astype(jnp.int32)
        q_first = lax.dynamic_slice_in_dim(q_nope, start, block, 0).astype(jnp.float32)
        q_second = lax.dynamic_slice_in_dim(q_rope, start, block, 0).astype(jnp.float32)
        scores = jnp.einsum('qhd,khd->hqk', q_first, key_all) + jnp.einsum('qhr,kr->hqk', q_second, rot_all)
        scores = scores * scale
        query_pos = start + jnp.arange(block, dtype=jnp.int32)
        mask = key_pos[None, :] <= query_pos[:, None]
        top = lax.optimization_barrier(jnp.max(jnp.where(mask[None], scores, -jnp.inf), axis=-1, keepdims=True))
        expo = jnp.where(mask[None], jnp.exp(scores - top), 0.0)
        total = lax.optimization_barrier(jnp.sum(expo, axis=-1))
        weighted = jnp.einsum('hqk,khv->hqv', round_trip(expo), value_all)
        result = (weighted / total[..., None]).astype(jnp.bfloat16)
        return jnp.transpose(result, (1, 0, 2)).reshape(block, heads * vsize)
    blocks = lax.map(one_block, jnp.arange(length // block, dtype=jnp.int32))
    return blocks.reshape(length, heads * vsize)

def reference(residual, query_a, query_b, latents, rope_key, key_up_a, value_up_a, key_up_b, value_up_b, out_proj_a, out_proj_b, norm_gain, routes, route_weights, shared_gate, shared_up, shared_down, expert_gate, expert_up, expert_down):
    positions = jnp.arange(TOKENS, dtype=jnp.int32)
    cosine, sine = tables(positions)
    rot_key = rotate(rope_key, cosine, sine)
    keys_a = jnp.dot(latents, key_up_a, preferred_element_type=jnp.float32).astype(jnp.bfloat16)
    values_a = jnp.dot(latents, value_up_a, preferred_element_type=jnp.float32).astype(jnp.bfloat16)
    keys_b = jnp.dot(latents, key_up_b, preferred_element_type=jnp.float32).astype(jnp.bfloat16)
    values_b = jnp.dot(latents, value_up_b, preferred_element_type=jnp.float32).astype(jnp.bfloat16)
    heads_a = attend(query_a, keys_a, values_a, rot_key, HA, DA, VA, cosine, sine)
    heads_b = attend(query_b, keys_b, values_b, rot_key, HB, DB, VB, cosine, sine)
    width_a = HA * VA // N_TP
    width_b = HB * VB // N_TP

    def head_block(total, index):
        part = jnp.dot(lax.dynamic_slice_in_dim(heads_a, index * width_a, width_a, 1), lax.dynamic_slice_in_dim(out_proj_a, index * width_a, width_a, 0), preferred_element_type=jnp.float32)
        part = part + jnp.dot(lax.dynamic_slice_in_dim(heads_b, index * width_b, width_b, 1), lax.dynamic_slice_in_dim(out_proj_b, index * width_b, width_b, 0), preferred_element_type=jnp.float32)
        return (total + round_trip(part), None)
    mixed, _ = lax.scan(head_block, jnp.zeros((TOKENS, D), jnp.float32), jnp.arange(N_TP, dtype=jnp.int32))
    hidden_state = (residual.astype(jnp.float32) + mixed).astype(jnp.bfloat16)
    wide = hidden_state.astype(jnp.float32)
    normed = (wide * lax.rsqrt(lax.optimization_barrier(jnp.mean(wide * wide, axis=-1, keepdims=True)) + norm_eps) * norm_gain.astype(jnp.float32)).astype(jnp.bfloat16)
    flat = routes.reshape(-1).astype(jnp.int32)
    owners = jnp.arange(TOKENS * TOPK, dtype=jnp.int32) // TOPK
    weights_flat = route_weights.reshape(-1).astype(jnp.float32)
    bound = N_SP * CAP

    def select(expert):
        order = jnp.argsort(jnp.where(flat == expert, 0, 1).astype(jnp.int32), stable=True)[:bound].astype(jnp.int32)
        chosen = jnp.where(flat[order] == expert, weights_flat[order], 0.0)
        return (owners[order], chosen)
    rows_of, weight_of = lax.map(select, jnp.arange(EXPERTS, dtype=jnp.int32))
    expert_width = EXPERT_FF // N_TP
    shared_width = SHARED_FF // N_TP

    def width_block(total, index):
        s_gate = lax.dynamic_slice_in_dim(shared_gate, index * shared_width, shared_width, 1)
        s_up = lax.dynamic_slice_in_dim(shared_up, index * shared_width, shared_width, 1)
        s_down = lax.dynamic_slice_in_dim(shared_down, index * shared_width, shared_width, 0)
        act = (jax.nn.silu(jnp.dot(normed, s_gate, preferred_element_type=jnp.float32)) * jnp.dot(normed, s_up, preferred_element_type=jnp.float32)).astype(jnp.bfloat16)
        term = jnp.dot(act, s_down, preferred_element_type=jnp.float32)

        def one_expert(acc, pieces):
            gate_w, up_w, down_w, rows, weight = pieces
            taken = normed[rows]
            gate_blk = lax.dynamic_slice_in_dim(gate_w, index * expert_width, expert_width, 1)
            up_blk = lax.dynamic_slice_in_dim(up_w, index * expert_width, expert_width, 1)
            down_blk = lax.dynamic_slice_in_dim(down_w, index * expert_width, expert_width, 0)
            act_e = (jax.nn.silu(jnp.dot(taken, gate_blk, preferred_element_type=jnp.float32)) * jnp.dot(taken, up_blk, preferred_element_type=jnp.float32)).astype(jnp.bfloat16)
            part = round_trip(jnp.dot(act_e, down_blk, preferred_element_type=jnp.float32))
            return (acc.at[rows].add(part * weight[:, None]), None)
        term, _ = lax.scan(one_expert, term, (expert_gate, expert_up, expert_down, rows_of, weight_of))
        return (total + round_trip(term), None)
    moe, _ = lax.scan(width_block, jnp.zeros((TOKENS, D), jnp.float32), jnp.arange(N_TP, dtype=jnp.int32))
    return (hidden_state.astype(jnp.float32) + moe).astype(jnp.bfloat16)
```

```python
import functools

import jax
import jax.numpy as jnp
from jax import lax
from jax.experimental import pallas as pl
from jax.experimental.pallas import tpu as pltpu
from jax.sharding import PartitionSpec as P

DA = 64
VA = 64
DB = 128
VB = 128
ROPE = 32


theta_base = 10000.0
norm_eps = 1e-06
very_low = -1e30


def tables(positions, width):
    half = width // 2
    freqs = theta_base ** (-(2.0 * jnp.arange(half, dtype=jnp.float32)) / width)
    angles = positions.astype(jnp.float32)[:, None] * freqs[None, :]
    return (jnp.cos(angles), jnp.sin(angles))


def rotate(values, cosine, sine):
    half = values.shape[-1] // 2
    first = values[..., :half].astype(jnp.float32)
    second = values[..., half:].astype(jnp.float32)
    turned = jnp.concatenate(
        [first * cosine - second * sine, first * sine + second * cosine], axis=-1
    )
    return turned.astype(jnp.bfloat16)


def head_kernel(
    qa_ref, qb_ref, lat_ref, rota_ref, rotb_ref, kua_ref, vua_ref, kub_ref, vub_ref,
    qpos_ref, kpos_ref, out_ref, *, scale_a, scale_b
):
    mask = kpos_ref[...] <= qpos_ref[...]
    lat = lat_ref[...]

    def attend(queries, keys, values, scale):
        scores = lax.dot_general(
            queries, keys, (((1,), (1,)), ((), ())), preferred_element_type=jnp.float32
        )
        scores = jnp.where(mask, scores, very_low)
        top = jnp.max(scores, axis=-1, keepdims=True)
        expo = jnp.exp((scores - top) * scale)
        total = jnp.sum(expo, axis=-1, keepdims=True)
        weighted = jnp.dot(expo.astype(jnp.bfloat16), values, preferred_element_type=jnp.float32)
        return (weighted / total).astype(jnp.bfloat16)

    def project(weights):
        return jnp.dot(lat, weights, preferred_element_type=jnp.float32).astype(jnp.bfloat16)

    wide_a = kua_ref.shape[2]
    wide_v = vua_ref.shape[2]
    count_a = qa_ref.shape[0]
    for h in range(count_a):
        keys = project(kua_ref[h]) + rota_ref[...]
        out_ref[:, h * wide_v : (h + 1) * wide_v] = attend(
            qa_ref[h], keys, project(vua_ref[h]), scale_a
        )
    base = count_a * wide_v
    wide_k = kub_ref.shape[1] // qb_ref.shape[0]
    wide_v = vub_ref.shape[1] // qb_ref.shape[0]
    for h in range(qb_ref.shape[0]):
        keys = project(kub_ref[:, h * wide_k : (h + 1) * wide_k])
        keys = jnp.concatenate([keys, rotb_ref[...]], axis=1)
        out_ref[:, base + h * wide_v : base + (h + 1) * wide_v] = attend(
            qb_ref[h], keys, project(vub_ref[:, h * wide_v : (h + 1) * wide_v]), scale_b
        )


def padded_heads(weights, heads, lanes):
    split = weights.reshape(weights.shape[0], heads, -1)
    split = jnp.pad(split, ((0, 0), (0, 0), (0, lanes - split.shape[2])))
    return jnp.transpose(split, (1, 0, 2))


def swap(values, axis, b):
    return lax.ppermute(values, axis, [(i, i ^ (1 << b)) for i in range(lax.axis_size(axis))])


def join(values, axis, b, dim):
    other = swap(values, axis, b)
    low = ((lax.axis_index(axis) >> b) & 1) == 0
    return jnp.concatenate(
        [jnp.where(low, values, other), jnp.where(low, other, values)], axis=dim
    )


def shards(
    residual,
    query_a,
    query_b,
    latents,
    rope_key,
    key_up_a,
    value_up_a,
    key_up_b,
    value_up_b,
    out_proj_a,
    out_proj_b,
    norm_gain,
    routes,
    route_weights,
    shared_gate,
    shared_up,
    shared_down,
    expert_gate,
    expert_up,
    expert_down,
):
    tok = query_a.shape[0]
    heads_a = key_up_a.shape[1] // DA
    heads_b = key_up_b.shape[1] // DB
    width = residual.shape[1]
    columns = Columns(width)
    sp_bits = lax.axis_size("sp").bit_length() - 1
    tp_bits = lax.axis_size("tp").bit_length() - 1

    rank = latents.shape[1]
    lanes = rank // lax.axis_size("tp")
    half = tok // 2
    piece = lax.dynamic_slice_in_dim(latents, columns.block * lanes, lanes, 1)
    packed = rope_key.reshape(tok * ROPE // lanes, lanes)
    one = jnp.concatenate([piece[:half], packed], axis=0)[None]
    two = piece[None, half:]
    order = list(range(1, sp_bits)) + [0]
    for b in order[:-1]:
        one = join(one, "sp", b, 0)
        two = join(two, "sp", b, 0)
    one = join(one, "sp", 0, 0)
    rope_rows = one[:, half:].reshape(-1, ROPE)
    one = one[:, :half]
    for b in reversed(range(1, tp_bits)):
        two = join(two, "tp", b, 2)
        one = join(one, "tp", b, 2)
    two = join(two, "sp", 0, 0)
    one = join(one, "tp", 0, 2)
    two = join(two, "tp", 0, 2)
    lat_rows = jnp.concatenate([one, two], axis=1).reshape(-1, rank)
    blocks = jnp.arange(lax.axis_size("sp"), dtype=jnp.int32)
    blocks = sum(((blocks >> j) & 1) << b for j, b in enumerate(order))
    key_pos = (blocks[:, None] * tok + jnp.arange(tok, dtype=jnp.int32)[None, :]).reshape(-1)

    query_pos = lax.axis_index("sp") * tok + jnp.arange(tok, dtype=jnp.int32)
    cosine, sine = tables(query_pos, ROPE)
    shaped_a = query_a.reshape(tok, heads_a, DA + ROPE)
    shaped_b = query_b.reshape(tok, heads_b, DB + ROPE)
    turned_a = rotate(shaped_a[..., DA:], cosine[:, None, :], sine[:, None, :])
    turned_b = rotate(shaped_b[..., DB:], cosine[:, None, :], sine[:, None, :])
    wide_a = -(-(DA + ROPE) // 128) * 128
    wide_v = -(-VA // 128) * 128
    extra = -(-ROPE // 128) * 128 - ROPE
    whole_a = jnp.concatenate([shaped_a[..., :DA], turned_a], axis=2)
    whole_a = jnp.pad(whole_a, ((0, 0), (0, 0), (0, wide_a - DA - ROPE)))
    whole_b = jnp.concatenate([shaped_b[..., :DB], turned_b], axis=2)
    whole_b = jnp.pad(whole_b, ((0, 0), (0, 0), (0, extra)))
    all_cos, all_sin = tables(key_pos, ROPE)
    rot_piece = rotate(rope_rows, all_cos, all_sin)
    heads_out = pl.pallas_call(
        functools.partial(
            head_kernel, scale_a=(DA + ROPE) ** (-0.5), scale_b=(DB + ROPE) ** (-0.5)
        ),
        out_shape=jax.ShapeDtypeStruct((tok, heads_a * wide_v + heads_b * VB), jnp.bfloat16),
        compiler_params=pltpu.CompilerParams(vmem_limit_bytes=56 * 1024 * 1024),
    )(
        jnp.transpose(whole_a, (1, 0, 2)),
        jnp.transpose(whole_b, (1, 0, 2)),
        lat_rows,
        jnp.pad(rot_piece, ((0, 0), (DA, wide_a - DA - ROPE))),
        jnp.pad(rot_piece, ((0, 0), (0, extra))),
        padded_heads(key_up_a, heads_a, wide_a),
        padded_heads(value_up_a, heads_a, wide_v),
        key_up_b,
        value_up_b,
        query_pos[:, None],
        key_pos[None, :],
    )
    proj_a = out_proj_a.reshape(heads_a, VA, width)
    proj_a = jnp.pad(proj_a, ((0, 0), (0, wide_v - VA), (0, 0))).reshape(-1, width)
    proj = jnp.concatenate([proj_a, out_proj_b], axis=0)
    term = jnp.dot(heads_out, proj, preferred_element_type=jnp.float32).astype(jnp.bfloat16)
    mixed = columns.reduce(term)
    hidden_state = (columns.from_rows(residual).astype(jnp.float32) + mixed).astype(jnp.bfloat16)
    hidden = hidden_state.astype(jnp.float32)
    square = jnp.sum(hidden * hidden, axis=-1, keepdims=True)
    for b in range(tp_bits):
        square = square + swap(square, "tp", b)
    gain = lax.dynamic_slice_in_dim(norm_gain, columns.block * columns.size, columns.size, 0)
    normed = (hidden * lax.rsqrt(square / width + norm_eps) * gain).astype(jnp.bfloat16)
    whole_rows = columns.gather(normed)

    experts = lax.axis_size("sp")
    topk = routes.shape[1]
    capacity = max(2, 3 * tok * topk // (2 * experts))
    padded = -(-capacity // 8) * 8
    flat = routes.reshape(-1)
    onehot = (flat[:, None] == jnp.arange(experts, dtype=jnp.int32)[None, :]).astype(jnp.int32)
    before = jnp.cumsum(onehot, axis=0) - onehot
    rank = jnp.sum(before * onehot, axis=1)
    slots = (flat * padded + rank).reshape(tok, topk)
    places = jnp.arange(experts * padded, dtype=jnp.int32)
    chosen = [(slots[:, k, None] == places[None, :]).astype(jnp.bfloat16) for k in range(topk)]
    placing = sum(chosen[1:], chosen[0])

    outgoing = jnp.dot(placing.T, normed, preferred_element_type=jnp.float32)
    outgoing = outgoing.astype(jnp.bfloat16).reshape(experts, padded, columns.size)
    arrived = lax.all_to_all(outgoing, "sp", split_axis=0, concat_axis=0, tiled=True)
    rows_in = columns.gather(arrived.reshape(experts * padded, columns.size))
    shared_act = (
        jax.nn.silu(jnp.dot(whole_rows, shared_gate, preferred_element_type=jnp.float32))
        * jnp.dot(whole_rows, shared_up, preferred_element_type=jnp.float32)
    ).astype(jnp.bfloat16)
    shared_term = jnp.dot(shared_act, shared_down, preferred_element_type=jnp.float32)
    shared_own = columns.reduce(shared_term)
    act = (
        jax.nn.silu(jnp.dot(rows_in, expert_gate[0], preferred_element_type=jnp.float32))
        * jnp.dot(rows_in, expert_up[0], preferred_element_type=jnp.float32)
    ).astype(jnp.bfloat16)
    part = jnp.dot(act, expert_down[0], preferred_element_type=jnp.float32).astype(jnp.bfloat16)
    summed = columns.reduce(part).astype(jnp.bfloat16)
    back = lax.all_to_all(
        summed.reshape(experts, padded, columns.size), "sp", split_axis=0, concat_axis=0, tiled=True
    ).reshape(experts * padded, columns.size)
    moe = shared_own
    for k in range(topk):
        picked = jnp.dot(chosen[k], back, preferred_element_type=jnp.float32)
        moe = moe + picked * route_weights[:, k, None]
    return columns.to_rows((hidden + moe).astype(jnp.bfloat16))


class Columns:
    def __init__(self, width):
        count = lax.axis_size("tp")
        self.count = count
        self.bits = count.bit_length() - 1
        self.size = width // count
        self.index = lax.axis_index("tp")
        self.block = sum(
            ((self.index >> b) & 1) << (self.bits - 1 - b) for b in range(self.bits)
        )

    def of(self, device):
        return sum(((device >> b) & 1) << (self.bits - 1 - b) for b in range(self.bits))

    def gather(self, values):
        for b in reversed(range(self.bits)):
            values = join(values, "tp", b, 1)
        return values

    def reduce(self, values):
        for b in range(self.bits):
            half = values.shape[1] // 2
            bit = (self.index >> b) & 1
            first, second = values[:, :half], values[:, half:]
            sent = jnp.where(bit == 0, second, first).astype(jnp.bfloat16)
            kept = jnp.where(bit == 0, first, second).astype(jnp.float32)
            values = kept + swap(sent, "tp", b).astype(jnp.float32)
        return values

    def trade(self, piece_for, step):
        pairs = [(i, i ^ step) for i in range(self.count)]
        piece = piece_for(self.index ^ step)
        return piece if step == 0 else lax.ppermute(piece, "tp", pairs)

    def from_rows(self, values):
        rows = values.shape[0]
        result = jnp.zeros((rows * self.count, self.size), values.dtype)
        for step in range(self.count):
            piece = self.trade(
                lambda d: lax.dynamic_slice_in_dim(values, self.of(d) * self.size, self.size, 1),
                step,
            )
            result = lax.dynamic_update_slice_in_dim(result, piece, (self.index ^ step) * rows, 0)
        return result

    def to_rows(self, values):
        rows = values.shape[0] // self.count
        result = jnp.zeros((rows, self.size * self.count), values.dtype)
        for step in range(self.count):
            piece = self.trade(lambda d: lax.dynamic_slice_in_dim(values, d * rows, rows, 0), step)
            start = self.of(self.index ^ step) * self.size
            result = lax.dynamic_update_slice_in_dim(result, piece, start, 1)
        return result


def solution(mesh):
    placed = (
        P(("sp", "tp"), None),
        P("sp", "tp"),
        P("sp", "tp"),
        P("sp", None),
        P("sp", None),
        P(None, "tp"),
        P(None, "tp"),
        P(None, "tp"),
        P(None, "tp"),
        P("tp", None),
        P("tp", None),
        P(),
        P("sp", None),
        P("sp", None),
        P(None, "tp"),
        P(None, "tp"),
        P("tp", None),
        P("sp", None, "tp"),
        P("sp", None, "tp"),
        P("sp", "tp", None),
    )
    return jax.shard_map(
        shards, mesh=mesh, in_specs=placed, out_specs=P(("sp", "tp"), None), check_vma=False
    )
```
